256 devices in a mesh: grp: 2 (over y), fs: 16 (over z), tp: 8 (over x, core).
Axes of the slice: x: 4, y: 2, z: 16, core: 2. Of those that a mesh axis runs over, the one named last changes fastest.
The devices are a block of a 4x16x16 slice.
Arguments:
- prompt_rows: bfloat16 [32768, 2048], P(('grp', 'fs')), parts along dimension 0, may hold values from -6 to 6
- up_master: float32 [2048, 8192], P('fs', 'tp'), may hold values from -0.125 to 0.125
- down_master: float32 [8192, 2048], P('fs', 'tp'), may hold values from -0.0625 to 0.0625
- norm_gain: float32 [2048], P('fs'), may hold values from 0.1 to 1.9
Outputs:
- up_sampler: bfloat16 [16, 2048, 1024], P(('grp', 'tp')), parts along dimension 0
- down_sampler: bfloat16 [16, 1024, 2048], P(('grp', 'tp')), parts along dimension 0
- layer_out: bfloat16 [32768, 2048], P(('grp', 'fs', 'tp')), parts along dimension 0
The draws below stay inside these ranges and needn't reach their ends.
There are 2 independent parts, one for each index of `grp`. The reference program is written for one: setup_inputs(seed, part) draws one part's arguments, and reference() takes and returns one part's arrays. A program takes and returns all parts, laid end to end along the dimension named above; an argument that names none is the same for every part. Nothing has to cross between parts.
All inputs are finite; a program needn't handle non-finite values.
Results may differ from the reference program's by a relative error of at most 0.014.
Values may be sent and summed in bfloat16 or wider, within the bound.
No kernel may reach another device: no remote copies, remote signals or barrier semaphores. Data moves between devices by JAX's collectives and lax.ppermute only.
A program may use at most 64 MiB of HBM per device.

```python
import jax
import jax.numpy as jnp
from jax import lax

D = 2048
FF = 8192
TOKENS = 16384
UNIT_SPAN = 64
N_FS = 16
N_TP = 8


def block_scale(rng, extent, split, low, largest):
    level, own = 1.0, jax.random.fold_in(rng, 6)
    for dim, blocks in split:
        steps = jnp.exp(jax.random.uniform(jax.random.fold_in(own, dim), (blocks,), jnp.float32, low / len(split), largest / len(split)))
        level = level * jnp.repeat(steps, extent[dim] // blocks).reshape([-1 if axis == dim else 1 for axis in range(len(extent))])
    return level


def noise(stream_key, shape, width, reach, cuts=(), kind=jnp.bfloat16):
    gain = block_scale(stream_key, shape, cuts, -0.22, 0.18) if cuts else 1.0
    drawn = jax.random.normal(stream_key, shape, jnp.float32) * width * gain
    return jnp.minimum(jnp.maximum(drawn, -reach), reach).astype(kind)


def setup_inputs(seed: int = 0, part: int = 0) -> dict:
    key_of = jax.random.split(jax.random.key(seed), 5)
    part_splits = jax.random.split(jax.random.fold_in(key_of[4], part), 5)
    prompt_rows = noise(part_splits[0], (TOKENS, D), 1.0, 6.0, ((0, 16),))
    up_master = noise(key_of[1], (D, FF), D ** -0.5, 0.125, ((0, 16), (1, 8)), jnp.float32)
    down_master = noise(key_of[2], (FF, D), FF ** -0.5, 0.0625, ((0, 16), (1, 8)), jnp.float32)
    norm_gain = jnp.clip(1.0 + 0.18 * jax.random.normal(key_of[3], (D,), jnp.float32), 0.1, 1.9)
    return {"prompt_rows": prompt_rows, "up_master": up_master, "down_master": down_master, "norm_gain": norm_gain}


eps = 1e-06

def reference(prompt_rows, up_master, down_master, norm_gain):
    folded = (up_master * norm_gain[:, None]).astype(jnp.bfloat16)
    down_cast = down_master.astype(jnp.bfloat16)
    up_sampler = folded.reshape(D, N_FS, N_TP, UNIT_SPAN).transpose(2, 0, 1, 3).reshape(N_TP, D, N_FS * UNIT_SPAN)
    down_sampler = down_cast.reshape(N_FS, N_TP, UNIT_SPAN, D).transpose(1, 0, 2, 3).reshape(N_TP, N_FS * UNIT_SPAN, D)
    values = prompt_rows.astype(jnp.float32)
    normed = (values * lax.rsqrt(lax.optimization_barrier(jnp.mean(values * values, axis=-1, keepdims=True)) + eps)).astype(jnp.bfloat16)
    total = jnp.zeros((prompt_rows.shape[0], D), jnp.float32)
    for group in range(N_TP):
        pre_act = jnp.dot(normed, up_sampler[group], preferred_element_type=jnp.float32)
        hidden = jnp.square(jax.nn.relu(pre_act)).astype(jnp.bfloat16)
        partial_value = jnp.dot(hidden, down_sampler[group], preferred_element_type=jnp.float32).astype(jnp.bfloat16)
        partial_value = lax.optimization_barrier(partial_value)
        total = total + partial_value.astype(jnp.float32)
    return (up_sampler, down_sampler, total.astype(jnp.bfloat16))
```

```python
import jax
import jax.numpy as jnp
from jax import lax
from jax.sharding import PartitionSpec as P

eps = 1e-06


def on_device(prompt_rows, up_master, down_master, norm_gain):
    n_fs = lax.axis_size("fs")
    n_tp = lax.axis_size("tp")
    n_x = n_tp // 2
    z = lax.axis_index("fs")
    tp = lax.axis_index("tp")
    x = tp // 2
    core = tp % 2
    direction = 1 - 2 * core

    up_rows, width = up_master.shape
    span = width // n_fs
    per_tp = n_fs // n_tp
    down_cols = down_master.shape[1]
    full = down_cols * n_tp
    folds = down_cols // (per_tp * span)

    pair = [(k, k ^ 1) for k in range(n_tp)]
    ring = [
        (f * n_tp + k, (f + (1 if k % 2 == 0 else -1)) % n_fs * n_tp + k)
        for f in range(n_fs)
        for k in range(n_tp)
    ]

    up_cast = (up_master * norm_gain[:, None]).astype(jnp.bfloat16)
    down_cast = down_master.astype(jnp.bfloat16)
    up_parts = up_cast.reshape(up_rows, per_tp, n_tp, span).transpose(2, 0, 1, 3)
    up_parts = up_parts.reshape(n_tp, 1, up_rows, per_tp * span)
    down_parts = down_cast.reshape(n_tp, span, folds, per_tp * span).transpose(0, 2, 1, 3)
    down_parts = down_parts.reshape(n_tp, 1, folds * span, per_tp * span)
    parts = jnp.concatenate([up_parts, down_parts], axis=1)
    parts = lax.all_to_all(parts, "tp", split_axis=0, concat_axis=0, tiled=True)
    up_own = parts[:, 0].transpose(1, 0, 2).reshape(up_rows, width)
    down_own = parts[:, 1].reshape(n_tp, folds, span, per_tp * span).transpose(2, 0, 1, 3)
    down_own = down_own.reshape(span, full)

    up_msg = jnp.stack([up_own, lax.ppermute(up_own, "tp", pair)])
    down_msg = jnp.stack([down_own, lax.ppermute(down_own, "tp", pair)])

    up_out = jnp.zeros((n_fs, up_rows, width), jnp.bfloat16)
    down_out = jnp.zeros((n_fs, span, full), jnp.bfloat16)

    def put(out, block, at):
        return lax.dynamic_update_slice(out, block[None], (at, 0, 0))

    up_out = put(up_out, up_own, z)
    down_out = put(down_out, down_own, z)
    half = n_fs // 2
    for step in range(1, half + 1):
        back = (z + n_fs - step * direction) % n_fs
        ahead = (z + n_fs + step * direction) % n_fs
        if step < half:
            up_msg = lax.ppermute(up_msg, ("fs", "tp"), ring)
            down_msg = lax.ppermute(down_msg, ("fs", "tp"), ring)
            up_out = put(up_out, up_msg[0], back)
            up_out = put(up_out, lax.ppermute(up_msg[1], "tp", pair), ahead)
            down_out = put(down_out, down_msg[0], back)
            down_out = put(down_out, lax.ppermute(down_msg[1], "tp", pair), ahead)
        else:
            up_out = put(up_out, lax.ppermute(up_msg[0], ("fs", "tp"), ring), back)
            down_out = put(down_out, lax.ppermute(down_msg[0], ("fs", "tp"), ring), back)
    up_sampler = up_out.reshape(n_fs * up_rows, width)
    down_sampler = down_out.reshape(n_fs * span, full)

    values = prompt_rows.astype(jnp.float32)
    normed = (values * lax.rsqrt(jnp.mean(values * values, axis=-1, keepdims=True) + eps)).astype(
        jnp.bfloat16
    )
    pre_act = jnp.dot(normed, up_sampler, preferred_element_type=jnp.float32)
    hidden = jnp.square(jax.nn.relu(pre_act)).astype(jnp.bfloat16)

    tokens = prompt_rows.shape[0]
    chunks = 2
    cols = full // chunks
    sums = []
    for k in range(chunks):
        weights = lax.slice_in_dim(down_sampler, k * cols, (k + 1) * cols, axis=1)
        partial = jnp.dot(hidden, weights, preferred_element_type=jnp.float32).astype(jnp.bfloat16)
        partial = partial.reshape(n_x, 2, tokens // n_tp, cols)
        mine = lax.dynamic_index_in_dim(partial, core, 1, keepdims=False)
        other = lax.dynamic_index_in_dim(partial, 1 - core, 1, keepdims=False)
        other = lax.ppermute(other, "tp", pair)
        chip = mine.astype(jnp.float32) + other.astype(jnp.float32)
        total = lax.dynamic_index_in_dim(chip, x, 0, keepdims=False)
        chip = chip.astype(jnp.bfloat16)
        for far in range(1, n_x):
            block = lax.dynamic_index_in_dim(chip, (x + far) % n_x, 0, keepdims=False)
            perm = [(k2, (k2 + 2 * far) % n_tp) for k2 in range(n_tp)]
            total = total + lax.ppermute(block, "tp", perm).astype(jnp.float32)
        sums.append(total.astype(jnp.bfloat16))
    return (up_sampler[None], down_sampler[None], jnp.concatenate(sums, axis=1))


def solution(mesh):
    in_specs = (P(("grp", "fs"), None), P("fs", "tp"), P("fs", "tp"), P("fs"))
    out_specs = (
        P(("grp", "tp"), None, None),
        P(("grp", "tp"), None, None),
        P(("grp", "fs", "tp"), None),
    )
    return jax.shard_map(
        on_device, mesh=mesh, in_specs=in_specs, out_specs=out_specs, check_vma=False
    )
```

```python
import jax
import jax.numpy as jnp
from jax import lax
from jax.experimental import pallas as pl
from jax.experimental.pallas import tpu as pltpu
from jax.sharding import PartitionSpec as P

eps = 1e-06


def place(z, moves, outs, n_fs, earlier=None):
    pieces = []
    for move in moves:
        if not any(move[0] is piece for piece in pieces):
            pieces.append(move[0])
    at = [next(k for k, piece in enumerate(pieces) if piece is move[0]) for move in moves]
    n_old = 0 if earlier is None else len(earlier)

    def body(z_ref, *refs):
        ins = refs[: len(pieces)]
        out_refs = refs[len(pieces) + n_old : len(pieces) + n_old + len(outs)]
        sems = refs[-1]
        copies = []
        for k, (_, row, rows, out, offset, block, within, col) in enumerate(moves):
            home = lax.rem(z_ref[0] + (offset + n_fs), n_fs)
            start = pl.multiple_of(home * block + within, 16)
            src = ins[at[k]]
            dst = out_refs[out].at[pl.ds(start, rows), pl.ds(col, src.shape[1])]
            copies.append(pltpu.make_async_copy(src.at[pl.ds(row, rows)], dst, sems.at[k]))
        for copy in copies:
            copy.start()
        for copy in copies:
            copy.wait()

    anywhere = pl.BlockSpec(memory_space=pl.ANY)
    old = [] if earlier is None else list(earlier)
    return pl.pallas_call(
        body,
        out_shape=outs,
        in_specs=[pl.BlockSpec(memory_space=pltpu.SMEM)] + [anywhere] * (len(pieces) + n_old),
        out_specs=[anywhere] * len(outs),
        scratch_shapes=[pltpu.SemaphoreType.DMA((len(moves),))],
        input_output_aliases={1 + len(pieces) + k: k for k in range(n_old)},
    )(z.reshape(1), *pieces, *old)


def on_device(prompt_rows, up_master, down_master, norm_gain):
    n_fs = lax.axis_size("fs")
    n_tp = lax.axis_size("tp")
    n_x = n_tp // 2
    half = n_fs // 2
    z = lax.axis_index("fs")
    tp = lax.axis_index("tp")
    x = tp // 2
    core = tp % 2

    up_rows, width = up_master.shape
    span = width // n_fs
    per_tp = n_fs // n_tp
    piece = per_tp * span
    down_cols = down_master.shape[1]
    full = down_cols * n_tp
    folds = down_cols // piece
    sides = full // width

    up_cast = (up_master * norm_gain[:, None]).astype(jnp.bfloat16)
    down_cast = down_master.astype(jnp.bfloat16)
    up_parts = up_cast.reshape(up_rows, per_tp, n_tp, span).transpose(2, 0, 1, 3)
    up_parts = up_parts.reshape(n_tp, 1, up_rows, piece)
    down_parts = down_cast.reshape(n_tp, span, folds, piece).transpose(0, 2, 1, 3)
    down_parts = down_parts.reshape(n_tp, 1, folds * span, piece)
    parts = jnp.concatenate([up_parts, down_parts], axis=1)
    parts = lax.all_to_all(parts, "tp", split_axis=0, concat_axis=0, tiled=True)
    up_own = parts[:, 0].transpose(1, 0, 2).reshape(up_rows, width)
    down_own = parts[:, 1].reshape(sides, n_tp // sides, folds, span, piece)
    down_own = down_own.transpose(0, 3, 1, 2, 4).reshape(sides * span, width)
    own = jnp.concatenate([up_own, down_own], axis=0)

    fore = [(k, (k + 1) % n_fs) for k in range(n_fs)]
    back = [(k, (k - 1) % n_fs) for k in range(n_fs)]
    held = {0: own}
    for step in range(1, half):
        held[-step] = lax.ppermute(held[1 - step], "fs", fore)
        held[step] = lax.ppermute(held[step - 1], "fs", back)
    far_up = lax.ppermute(held[1 - half][:up_rows], "fs", fore)
    far_down = lax.ppermute(held[half - 1][up_rows:], "fs", back)

    def up_move(msg, offset):
        return (msg, 0, up_rows, 0, offset, up_rows, 0, 0)

    def down_moves(msg, row, offset):
        return [(msg, row + s * span, span, 1, offset, span, 0, s * width) for s in range(sides)]

    outs = [
        jax.ShapeDtypeStruct((n_fs * up_rows, width), jnp.bfloat16),
        jax.ShapeDtypeStruct((n_fs * span, full), jnp.bfloat16),
    ]
    early = [k for k in held if abs(k) < half - 1]
    late = [half - 1, 1 - half]
    blank = jnp.zeros((up_rows, width), jnp.bfloat16)
    moves = []
    for k in early:
        moves += [up_move(held[k], k)] + down_moves(held[k], up_rows, k)
    moves += [up_move(blank, k) for k in late + [half]]
    up_sampler, down_sampler = place(z, moves, outs, n_fs)

    values = prompt_rows.astype(jnp.float32)
    normed = (values * lax.rsqrt(jnp.mean(values * values, axis=-1, keepdims=True) + eps)).astype(
        jnp.bfloat16
    )
    normed = lax.optimization_barrier(normed)
    pre_act = jnp.dot(normed, up_sampler, preferred_element_type=jnp.float32)
    pre_act = lax.optimization_barrier(pre_act)

    moves = []
    for k in late:
        moves += [up_move(held[k], k)] + down_moves(held[k], up_rows, k)
    moves += [up_move(far_up, half)] + down_moves(far_down, 0, half)
    up_sampler, down_sampler = place(z, moves, outs, n_fs, (up_sampler, down_sampler))
    rest = jnp.concatenate([held[late[0]][:up_rows], held[late[1]][:up_rows], far_up], axis=0)
    features = [
        lax.dynamic_slice_in_dim(normed, (z + n_fs + k) % n_fs * up_rows, up_rows, axis=1)
        for k in late + [half]
    ]
    features = jnp.concatenate(features, axis=1)
    pre_act = pre_act + jnp.dot(features, rest, preferred_element_type=jnp.float32)
    hidden = jnp.square(jax.nn.relu(pre_act)).astype(jnp.bfloat16)

    pair = [(k, k ^ 1) for k in range(n_tp)]
    tokens = prompt_rows.shape[0]
    chunks = 2
    cols = full // chunks
    sums = []
    for k in range(chunks):
        weights = lax.slice_in_dim(down_sampler, k * cols, (k + 1) * cols, axis=1)
        partial = jnp.dot(hidden, weights, preferred_element_type=jnp.float32).astype(jnp.bfloat16)
        partial = partial.reshape(n_x, 2, tokens // n_tp, cols)
        mine = lax.dynamic_index_in_dim(partial, core, 1, keepdims=False)
        other = lax.dynamic_index_in_dim(partial, 1 - core, 1, keepdims=False)
        other = lax.ppermute(other, "tp", pair)
        chip = mine.astype(jnp.float32) + other.astype(jnp.float32)
        total = lax.dynamic_index_in_dim(chip, x, 0, keepdims=False)
        chip = chip.astype(jnp.bfloat16)
        for far in range(1, n_x):
            block = lax.dynamic_index_in_dim(chip, (x + far) % n_x, 0, keepdims=False)
            perm = [(j, (j + 2 * far) % n_tp) for j in range(n_tp)]
            total = total + lax.ppermute(block, "tp", perm).astype(jnp.float32)
        sums.append(total.astype(jnp.bfloat16))
    return (up_sampler[None], down_sampler[None], jnp.concatenate(sums, axis=1))


def solution(mesh):
    in_specs = (P(("grp", "fs"), None), P("fs", "tp"), P("fs", "tp"), P("fs"))
    out_specs = (
        P(("grp", "tp"), None, None),
        P(("grp", "tp"), None, None),
        P(("grp", "fs", "tp"), None),
    )
    return jax.shard_map(
        on_device, mesh=mesh, in_specs=in_specs, out_specs=out_specs, check_vma=False
    )
```

```python
import jax
import jax.numpy as jnp
from jax import lax
from jax.experimental import pallas as pl
from jax.experimental.pallas import tpu as pltpu
from jax.sharding import PartitionSpec as P

eps = 1e-06


def place(z, moves, outs, n_fs, earlier=None):
    pieces = []
    for move in moves:
        if not any(move[0] is piece for piece in pieces):
            pieces.append(move[0])
    at = [next(k for k, piece in enumerate(pieces) if piece is move[0]) for move in moves]
    n_old = 0 if earlier is None else len(earlier)

    def body(z_ref, *refs):
        ins = refs[: len(pieces)]
        out_refs = refs[len(pieces) + n_old : len(pieces) + n_old + len(outs)]
        sems = refs[-1]
        copies = []
        for k, (_, row, rows, out, offset, block, within, col) in enumerate(moves):
            home = lax.rem(z_ref[0] + (offset + n_fs), n_fs)
            start = pl.multiple_of(home * block + within, 16)
            src = ins[at[k]]
            dst = out_refs[out].at[pl.ds(start, rows), pl.ds(col, src.shape[1])]
            copies.append(pltpu.make_async_copy(src.at[pl.ds(row, rows)], dst, sems.at[k]))
        for copy in copies:
            copy.start()
        for copy in copies:
            copy.wait()

    anywhere = pl.BlockSpec(memory_space=pl.ANY)
    old = [] if earlier is None else list(earlier)
    return pl.pallas_call(
        body,
        out_shape=outs,
        in_specs=[pl.BlockSpec(memory_space=pltpu.SMEM)]
        + [pl.BlockSpec(memory_space=pltpu.VMEM)] * len(pieces)
        + [anywhere] * n_old,
        out_specs=[anywhere] * len(outs),
        scratch_shapes=[pltpu.SemaphoreType.DMA((len(moves),))],
        input_output_aliases={1 + len(pieces) + k: k for k in range(n_old)},
    )(z.reshape(1), *pieces, *old)


def on_device(prompt_rows, up_master, down_master, norm_gain):
    n_fs = lax.axis_size("fs")
    n_tp = lax.axis_size("tp")
    n_x = n_tp // 2
    half = n_fs // 2
    z = lax.axis_index("fs")
    tp = lax.axis_index("tp")
    x = tp // 2
    core = tp % 2

    up_rows, width = up_master.shape
    span = width // n_fs
    per_tp = n_fs // n_tp
    piece = per_tp * span
    down_cols = down_master.shape[1]
    full = down_cols * n_tp
    folds = down_cols // piece
    sides = full // width

    up_cast = (up_master * norm_gain[:, None]).astype(jnp.bfloat16)
    down_cast = down_master.astype(jnp.bfloat16)
    up_parts = up_cast.reshape(up_rows, per_tp, n_tp, span).transpose(2, 0, 1, 3)
    up_parts = up_parts.reshape(n_tp, 1, up_rows, piece)
    down_parts = down_cast.reshape(n_tp, span, folds, piece).transpose(0, 2, 1, 3)
    down_parts = down_parts.reshape(n_tp, 1, folds * span, piece)
    parts = jnp.concatenate([up_parts, down_parts], axis=1)
    parts = lax.all_to_all(parts, "tp", split_axis=0, concat_axis=0, tiled=True)
    up_own = parts[:, 0].transpose(1, 0, 2).reshape(up_rows, width)
    down_own = parts[:, 1].reshape(sides, n_tp // sides, folds, span, piece)
    down_own = down_own.transpose(0, 3, 1, 2, 4).reshape(sides * span, width)
    own = jnp.concatenate([up_own, down_own], axis=0)

    fore = [(k, (k + 1) % n_fs) for k in range(n_fs)]
    back = [(k, (k - 1) % n_fs) for k in range(n_fs)]
    held = {0: own}
    for step in range(1, half):
        held[-step] = lax.ppermute(held[1 - step], "fs", fore)
        held[step] = lax.ppermute(held[step - 1], "fs", back)
    far_up = lax.ppermute(held[1 - half][:up_rows], "fs", fore)
    far_down = lax.ppermute(held[half - 1][up_rows:], "fs", back)

    def up_move(msg, offset):
        return (msg, 0, up_rows, 0, offset, up_rows, 0, 0)

    def down_moves(msg, row, offset):
        return [(msg, row + s * span, span, 1, offset, span, 0, s * width) for s in range(sides)]

    outs = [
        jax.ShapeDtypeStruct((n_fs * up_rows, width), jnp.bfloat16),
        jax.ShapeDtypeStruct((n_fs * span, full), jnp.bfloat16),
    ]
    early = [k for k in held if abs(k) < half - 1]
    late = [half - 1, 1 - half]
    blank = jnp.zeros((up_rows, width), jnp.bfloat16)
    moves = []
    for k in early:
        moves += [up_move(held[k], k)] + down_moves(held[k], up_rows, k)
    moves += [up_move(blank, k) for k in late + [half]]
    up_sampler, down_sampler = place(z, moves, outs, n_fs)

    values = prompt_rows.astype(jnp.float32)
    normed = (values * lax.rsqrt(jnp.mean(values * values, axis=-1, keepdims=True) + eps)).astype(
        jnp.bfloat16
    )
    normed = lax.optimization_barrier(normed)
    pre_act = jnp.dot(normed, up_sampler, preferred_element_type=jnp.float32)
    pre_act = lax.optimization_barrier(pre_act)

    moves = []
    for k in late:
        moves += [up_move(held[k], k)] + down_moves(held[k], up_rows, k)
    moves += [up_move(far_up, half)] + down_moves(far_down, 0, half)
    up_sampler, down_sampler = place(z, moves, outs, n_fs, (up_sampler, down_sampler))
    rest = jnp.concatenate([held[late[0]][:up_rows], held[late[1]][:up_rows], far_up], axis=0)
    features = [
        lax.dynamic_slice_in_dim(normed, (z + n_fs + k) % n_fs * up_rows, up_rows, axis=1)
        for k in late + [half]
    ]
    features = jnp.concatenate(features, axis=1)
    pre_act = pre_act + jnp.dot(features, rest, preferred_element_type=jnp.float32)
    hidden = jnp.square(jax.nn.relu(pre_act)).astype(jnp.bfloat16)

    pair = [(k, k ^ 1) for k in range(n_tp)]
    tokens = prompt_rows.shape[0]
    chunks = 2
    cols = full // chunks
    sums = []
    for k in range(chunks):
        weights = lax.slice_in_dim(down_sampler, k * cols, (k + 1) * cols, axis=1)
        partial = jnp.dot(hidden, weights, preferred_element_type=jnp.float32).astype(jnp.bfloat16)
        partial = partial.reshape(n_x, 2, tokens // n_tp, cols)
        mine = lax.dynamic_index_in_dim(partial, core, 1, keepdims=False)
        other = lax.dynamic_index_in_dim(partial, 1 - core, 1, keepdims=False)
        other = lax.ppermute(other, "tp", pair)
        chip = mine.astype(jnp.float32) + other.astype(jnp.float32)
        total = lax.dynamic_index_in_dim(chip, x, 0, keepdims=False)
        chip = chip.astype(jnp.bfloat16)
        for far in range(1, n_x):
            block = lax.dynamic_index_in_dim(chip, (x + far) % n_x, 0, keepdims=False)
            perm = [(j, (j + 2 * far) % n_tp) for j in range(n_tp)]
            total = total + lax.ppermute(block, "tp", perm).astype(jnp.float32)
        sums.append(total.astype(jnp.bfloat16))
    return (up_sampler[None], down_sampler[None], jnp.concatenate(sums, axis=1))


def solution(mesh):
    in_specs = (P(("grp", "fs"), None), P("fs", "tp"), P("fs", "tp"), P("fs"))
    out_specs = (
        P(("grp", "tp"), None, None),
        P(("grp", "tp"), None, None),
        P(("grp", "fs", "tp"), None),
    )
    return jax.shard_map(
        on_device, mesh=mesh, in_specs=in_specs, out_specs=out_specs, check_vma=False
    )
```

```python
import jax
import jax.numpy as jnp
from jax import lax
from jax.experimental import pallas as pl
from jax.experimental.pallas import tpu as pltpu
from jax.sharding import PartitionSpec as P


eps = 1e-06


def place(z, moves, outs, n_fs, earlier=None):
    pieces = []
    for move in moves:
        if not any(move[0] is piece for piece in pieces):
            pieces.append(move[0])
    at = [next(k for k, piece in enumerate(pieces) if piece is move[0]) for move in moves]
    n_old = 0 if earlier is None else len(earlier)

    def body(z_ref, *refs):
        ins = refs[: len(pieces)]
        out_refs = refs[len(pieces) + n_old : len(pieces) + n_old + len(outs)]
        sems = refs[-1]
        copies = []
        for k, (_, row, rows, out, offset, block, within, col) in enumerate(moves):
            home = lax.rem(z_ref[0] + (offset + n_fs), n_fs)
            start = pl.multiple_of(home * block + within, 16)
            src = ins[at[k]]
            dst = out_refs[out].at[pl.ds(start, rows), pl.ds(col, src.shape[1])]
            copies.append(pltpu.make_async_copy(src.at[pl.ds(row, rows)], dst, sems.at[k]))
        for copy in copies:
            copy.start()
        for copy in copies:
            copy.wait()

    anywhere = pl.BlockSpec(memory_space=pl.ANY)
    old = [] if earlier is None else list(earlier)
    return pl.pallas_call(
        body,
        out_shape=outs,
        in_specs=[pl.BlockSpec(memory_space=pltpu.SMEM)]
        + [pl.BlockSpec(memory_space=pltpu.VMEM)] * len(pieces)
        + [anywhere] * n_old,
        out_specs=[anywhere] * len(outs),
        scratch_shapes=[pltpu.SemaphoreType.DMA((len(moves),))],
        input_output_aliases={1 + len(pieces) + k: k for k in range(n_old)},
    )(z.reshape(1), *pieces, *old)


def on_device(prompt_rows, up_master, down_master, norm_gain):
    n_fs = lax.axis_size("fs")
    n_tp = lax.axis_size("tp")
    n_x = n_tp // 2
    half = n_fs // 2
    z = lax.axis_index("fs")
    tp = lax.axis_index("tp")
    x = tp // 2
    core = tp % 2

    up_rows, width = up_master.shape
    span = width // n_fs
    per_tp = n_fs // n_tp
    piece = per_tp * span
    down_cols = down_master.shape[1]
    full = down_cols * n_tp
    folds = down_cols // piece
    sides = full // width

    up_cast = (up_master * norm_gain[:, None]).astype(jnp.bfloat16)
    down_cast = down_master.astype(jnp.bfloat16)
    up_parts = up_cast.reshape(up_rows, per_tp, n_tp, span).transpose(2, 0, 1, 3)
    up_parts = up_parts.reshape(n_tp, 1, up_rows, piece)
    down_parts = down_cast.reshape(n_tp, span, folds, piece).transpose(0, 2, 1, 3)
    down_parts = down_parts.reshape(n_tp, 1, folds * span, piece)
    parts = jnp.concatenate([up_parts, down_parts], axis=1)
    parts = lax.all_to_all(parts, "tp", split_axis=0, concat_axis=0, tiled=True)
    up_own = parts[:, 0].transpose(1, 0, 2).reshape(up_rows, width)
    down_own = parts[:, 1].reshape(sides, n_tp // sides, folds, span, piece)
    down_own = down_own.transpose(0, 3, 1, 2, 4).reshape(sides * span, width)

    own = jnp.concatenate([up_own, down_own], axis=0)

    fore = [(k, (k + 1) % n_fs) for k in range(n_fs)]
    back = [(k, (k - 1) % n_fs) for k in range(n_fs)]
    held = {0: own}
    for step in range(1, half):
        held[-step] = lax.ppermute(held[1 - step], "fs", fore)
        held[step] = lax.ppermute(held[step - 1], "fs", back)
    up_far = lax.ppermute(held[1 - half][:up_rows], "fs", fore)
    down_far = lax.ppermute(held[half - 1][up_rows:], "fs", back)

    def up_moves(keys):
        return [(held[k], 0, up_rows, 0, k, up_rows, 0, 0) for k in keys]

    def down_moves(keys):
        return [
            (held[k], up_rows + s * span, span, 0, k, span, 0, s * width)
            for k in keys
            for s in range(sides)
        ]

    near = half - 3
    early = [k for k in held if abs(k) <= near]
    late = [k for k in held if abs(k) > near]
    up_shape = [jax.ShapeDtypeStruct((n_fs * up_rows, width), jnp.bfloat16)]
    down_shape = [jax.ShapeDtypeStruct((n_fs * span, full), jnp.bfloat16)]
    blank = jnp.zeros((up_rows, width), jnp.bfloat16)
    moves = up_moves(early)
    moves += [(blank, 0, up_rows, 0, k, up_rows, 0, 0) for k in late + [half]]
    up_sampler = place(z, moves, up_shape, n_fs)
    down_sampler = place(z, down_moves(early), down_shape, n_fs)

    tokens = prompt_rows.shape[0]
    block = tokens // n_tp
    order = [(dx % n_x, dc) for dc in (1, 0) for dx in range(1, n_x + 1)]
    rows = [
        lax.dynamic_slice_in_dim(
            prompt_rows, ((x + dx) % n_x * 2 + (core + dc) % 2) * block, block, axis=0
        )
        for dx, dc in order
    ]
    values = lax.optimization_barrier(jnp.concatenate(rows, axis=0)).astype(jnp.float32)
    normed = (values * lax.rsqrt(jnp.mean(values * values, axis=-1, keepdims=True) + eps)).astype(
        jnp.bfloat16
    )
    normed = lax.optimization_barrier(normed)
    pre_act = jnp.dot(normed, up_sampler[0], preferred_element_type=jnp.float32)
    pre_act = lax.optimization_barrier(pre_act)

    rest = [held[k][:up_rows] for k in late] + [up_far]
    rest = jnp.concatenate(rest, axis=0)
    features = [
        lax.dynamic_slice_in_dim(normed, (z + n_fs + k) % n_fs * up_rows, up_rows, axis=1)
        for k in late + [half]
    ]
    features = lax.optimization_barrier(jnp.concatenate(features, axis=1))
    pre_act = pre_act + jnp.dot(features, rest, preferred_element_type=jnp.float32)
    hidden = jnp.square(jax.nn.relu(pre_act)).astype(jnp.bfloat16)

    moves = down_moves(late)
    moves += [(down_far, k * span, span, 0, half, span, 0, k * width) for k in range(sides)]
    down_sampler = place(z, moves, down_shape, n_fs, down_sampler)[0]
    moves = up_moves(late)
    moves += [(up_far, 0, up_rows, 0, half, up_rows, 0, 0)]
    up_sampler = place(z, moves, up_shape, n_fs, up_sampler)[0]

    pair = [(k, k ^ 1) for k in range(n_tp)]
    hops = [[(j, (j + 2 * dx) % n_tp) for j in range(n_tp)] for dx in range(1, n_x)]
    bounds = [0, 3 * full // 8, full]
    sums = []
    for lo, hi in zip(bounds[:-1], bounds[1:]):
        weights = lax.slice_in_dim(down_sampler, lo, hi, axis=1)
        partial = jnp.dot(hidden, weights, preferred_element_type=jnp.float32).astype(jnp.bfloat16)
        theirs = lax.ppermute(partial[: tokens // 2], "tp", pair)
        chip = partial[tokens // 2 :].astype(jnp.float32) + theirs.astype(jnp.float32)
        total = chip[(n_x - 1) * block :]
        chip = chip[: (n_x - 1) * block].astype(jnp.bfloat16)
        for k, hop in enumerate(hops):
            sent = chip[k * block : (k + 1) * block]
            total = total + lax.ppermute(sent, "tp", hop).astype(jnp.float32)
        sums.append(total.astype(jnp.bfloat16))
    return (up_sampler[None], down_sampler[None], jnp.concatenate(sums, axis=1))


def solution(mesh):
    in_specs = (P(("grp", "fs"), None), P("fs", "tp"), P("fs", "tp"), P("fs"))
    out_specs = (
        P(("grp", "tp"), None, None),
        P(("grp", "tp"), None, None),
        P(("grp", "fs", "tp"), None),
    )

    return jax.shard_map(
        on_device, mesh=mesh, in_specs=in_specs, out_specs=out_specs, check_vma=False
    )
```

```python
import jax
import jax.numpy as jnp
from jax import lax
from jax.experimental import pallas as pl
from jax.experimental.pallas import tpu as pltpu
from jax.sharding import PartitionSpec as P


eps = 1e-06


def place(z, moves, outs, n_fs, earlier=None):
    pieces = []
    for move in moves:
        if not any(move[0] is piece for piece in pieces):
            pieces.append(move[0])
    at = [next(k for k, piece in enumerate(pieces) if piece is move[0]) for move in moves]
    n_old = 0 if earlier is None else len(earlier)

    def body(z_ref, *refs):
        ins = refs[: len(pieces)]
        out_refs = refs[len(pieces) + n_old : len(pieces) + n_old + len(outs)]
        sems = refs[-1]
        copies = []
        for k, (_, row, rows, out, offset, block, within, col) in enumerate(moves):
            home = lax.rem(z_ref[0] + (offset + n_fs), n_fs)
            start = pl.multiple_of(home * block + within, 16)
            src = ins[at[k]]
            dst = out_refs[out].at[pl.ds(start, rows), pl.ds(col, src.shape[1])]
            copies.append(pltpu.make_async_copy(src.at[pl.ds(row, rows)], dst, sems.at[k]))
        for copy in copies:
            copy.start()
        for copy in copies:
            copy.wait()

    anywhere = pl.BlockSpec(memory_space=pl.ANY)
    old = [] if earlier is None else list(earlier)
    return pl.pallas_call(
        body,
        out_shape=outs,
        in_specs=[pl.BlockSpec(memory_space=pltpu.SMEM)]
        + [pl.BlockSpec(memory_space=pltpu.VMEM)] * len(pieces)
        + [anywhere] * n_old,
        out_specs=[anywhere] * len(outs),
        scratch_shapes=[pltpu.SemaphoreType.DMA((len(moves),))],
        input_output_aliases={1 + len(pieces) + k: k for k in range(n_old)},
    )(z.reshape(1), *pieces, *old)


def on_device(prompt_rows, up_master, down_master, norm_gain):
    n_fs = lax.axis_size("fs")
    n_tp = lax.axis_size("tp")
    n_x = n_tp // 2
    half = n_fs // 2
    z = lax.axis_index("fs")
    tp = lax.axis_index("tp")
    x = tp // 2
    core = tp % 2

    up_rows, width = up_master.shape
    span = width // n_fs
    per_tp = n_fs // n_tp
    piece = per_tp * span
    down_cols = down_master.shape[1]
    full = down_cols * n_tp
    folds = down_cols // piece
    sides = full // width

    up_cast = (up_master * norm_gain[:, None]).astype(jnp.bfloat16)
    down_cast = down_master.astype(jnp.bfloat16)
    up_parts = up_cast.reshape(up_rows, per_tp, n_tp, span).transpose(2, 0, 1, 3)
    up_parts = up_parts.reshape(n_tp, 1, up_rows, piece)
    down_parts = down_cast.reshape(n_tp, span, folds, piece).transpose(0, 2, 1, 3)
    down_parts = down_parts.reshape(n_tp, 1, folds * span, piece)
    parts = jnp.concatenate([up_parts, down_parts], axis=1)
    parts = lax.all_to_all(parts, "tp", split_axis=0, concat_axis=0, tiled=True)
    up_own = parts[:, 0].transpose(1, 0, 2).reshape(up_rows, width)
    down_own = parts[:, 1].reshape(sides, n_tp // sides, folds, span, piece)
    down_own = down_own.transpose(0, 3, 1, 2, 4).reshape(sides * span, width)

    own = jnp.concatenate([up_own, down_own], axis=0)

    fore = [(k, (k + 1) % n_fs) for k in range(n_fs)]
    back = [(k, (k - 1) % n_fs) for k in range(n_fs)]
    held = {0: own}
    for step in range(1, half):
        held[-step] = lax.ppermute(held[1 - step], "fs", fore)
        held[step] = lax.ppermute(held[step - 1], "fs", back)
    up_far = lax.ppermute(held[1 - half][:up_rows], "fs", fore)
    down_far = lax.ppermute(held[half - 1][up_rows:], "fs", back)

    def up_moves(keys):
        return [(held[k], 0, up_rows, 0, k, up_rows, 0, 0) for k in keys]

    def down_moves(keys):
        return [
            (held[k], up_rows + s * span, span, 0, k, span, 0, s * width)
            for k in keys
            for s in range(sides)
        ]

    def within(least, most):
        return [k for k in held if least <= abs(k) <= most]

    late = [half - 2, half - 1, half, half + 1, half + 2]
    up_shape = [jax.ShapeDtypeStruct((n_fs * up_rows, width), jnp.bfloat16)]
    down_shape = [jax.ShapeDtypeStruct((n_fs * span, full), jnp.bfloat16)]
    blank = jnp.zeros((up_rows, width), jnp.bfloat16)
    moves = up_moves(within(0, half - 3))
    moves += [(blank, 0, up_rows, 0, k, up_rows, 0, 0) for k in late]
    up_sampler = place(z, moves, up_shape, n_fs)
    down_sampler = place(z, down_moves(within(0, half - 4)), down_shape, n_fs)
    moves = down_moves(within(half - 3, half - 2))
    down_sampler = place(z, moves, down_shape, n_fs, down_sampler)

    tokens = prompt_rows.shape[0]
    block = tokens // n_tp
    order = [(dx % n_x, dc) for dc in (1, 0) for dx in range(1, n_x + 1)]
    rows = [
        lax.dynamic_slice_in_dim(
            prompt_rows, ((x + dx) % n_x * 2 + (core + dc) % 2) * block, block, axis=0
        )
        for dx, dc in order
    ]
    values = lax.optimization_barrier(jnp.concatenate(rows, axis=0)).astype(jnp.float32)
    scale = lax.rsqrt(jnp.mean(values * values, axis=-1, keepdims=True) + eps)
    normed = lax.optimization_barrier((values * scale).astype(jnp.bfloat16))
    pre_act = jnp.dot(normed, up_sampler[0], preferred_element_type=jnp.float32)
    pre_act = lax.optimization_barrier(pre_act)

    rest = [up_far if k == half else held[k if k < half else k - n_fs][:up_rows] for k in late]
    rest = jnp.concatenate(rest, axis=0)
    ends = (len(late) - 1) * up_rows
    features = jnp.concatenate([normed, normed[:, :ends]], axis=1)
    features = lax.dynamic_slice_in_dim(
        features, (z + late[0]) % n_fs * up_rows, len(late) * up_rows, axis=1
    )
    features = lax.optimization_barrier(features)
    pre_act = pre_act + jnp.dot(features, rest, preferred_element_type=jnp.float32)
    hidden = jnp.square(jax.nn.relu(pre_act)).astype(jnp.bfloat16)

    moves = down_moves(within(half - 1, half - 1))
    moves += [(down_far, k * span, span, 0, half, span, 0, k * width) for k in range(sides)]
    down_sampler = place(z, moves, down_shape, n_fs, down_sampler)[0]
    moves = up_moves(within(half - 2, half - 1))
    moves += [(up_far, 0, up_rows, 0, half, up_rows, 0, 0)]
    up_sampler = place(z, moves, up_shape, n_fs, up_sampler)[0]

    pair = [(k, k ^ 1) for k in range(n_tp)]
    right = [(j, (j + 2) % n_tp) for j in range(n_tp)]
    left = [(j, (j - 2) % n_tp) for j in range(n_tp)]
    bounds = [0, 3 * full // 8, full]
    sums = []
    for lo, hi in zip(bounds[:-1], bounds[1:]):
        weights = lax.slice_in_dim(down_sampler, lo, hi, axis=1)
        partial = jnp.dot(hidden, weights, preferred_element_type=jnp.float32).astype(jnp.bfloat16)
        theirs = lax.ppermute(partial[: tokens // 2], "tp", pair)
        chip = partial[tokens // 2 :].astype(jnp.float32) + theirs.astype(jnp.float32)
        after, across, before, total = [chip[k * block : (k + 1) * block] for k in range(n_x)]
        across = across.astype(jnp.bfloat16)
        mid = (hi - lo) // 2
        first = lax.ppermute(across[:, :mid], "tp", right).astype(jnp.float32)
        second = lax.ppermute(across[:, mid:], "tp", left).astype(jnp.float32)
        after = jnp.concatenate([after[:, :mid] + first, after[:, mid:]], axis=1)
        before = jnp.concatenate([before[:, :mid], before[:, mid:] + second], axis=1)
        after = lax.ppermute(after.astype(jnp.bfloat16), "tp", right).astype(jnp.float32)
        before = lax.ppermute(before.astype(jnp.bfloat16), "tp", left).astype(jnp.float32)
        total = total + after + before
        sums.append(total.astype(jnp.bfloat16))
    return (up_sampler[None], down_sampler[None], jnp.concatenate(sums, axis=1))


def solution(mesh):
    in_specs = (P(("grp", "fs"), None), P("fs", "tp"), P("fs", "tp"), P("fs"))
    out_specs = (
        P(("grp", "tp"), None, None),
        P(("grp", "tp"), None, None),
        P(("grp", "fs", "tp"), None),
    )

    return jax.shard_map(
        on_device, mesh=mesh, in_specs=in_specs, out_specs=out_specs, check_vma=False
    )
```

```python
import jax
import jax.numpy as jnp
from jax import lax
from jax.experimental import pallas as pl
from jax.experimental.pallas import tpu as pltpu
from jax.sharding import PartitionSpec as P


eps = 1e-06


def place(home, moves, outs, n_fs, earlier=None):
    pieces = []
    used = []
    for piece, row, rows, *_ in moves:
        if not any(piece is known for known in pieces):
            pieces.append(piece)
            used.append(0)
        at = next(k for k, known in enumerate(pieces) if known is piece)
        used[at] = max(used[at], row + rows)
    where = [next(k for k, known in enumerate(pieces) if known is move[0]) for move in moves]
    n_old = 0 if earlier is None else 1

    def body(home_ref, *refs):
        ins = refs[: len(pieces)]
        out = refs[len(pieces) + n_old]
        sems = refs[-1]
        copies = []
        for k, (_, row, rows, offset, block, within, col) in enumerate(moves):
            slot = lax.rem(home_ref[0] + offset * home_ref[1] + n_fs, n_fs)
            start = pl.multiple_of(slot * block + within, 16)
            src = ins[where[k]]
            dst = out.at[pl.ds(start, rows), pl.ds(col, src.shape[1])]
            copies.append(pltpu.make_async_copy(src.at[pl.ds(row, rows)], dst, sems.at[k]))
        for copy in copies:
            copy.start()
        for copy in copies:
            copy.wait()

    anywhere = pl.BlockSpec(memory_space=pl.ANY)
    bands = [
        pl.BlockSpec((rows, piece.shape[1]), lambda _: (0, 0), memory_space=pltpu.VMEM)
        for piece, rows in zip(pieces, used)
    ]
    return pl.pallas_call(
        body,
        out_shape=outs,
        grid=(1,),
        in_specs=[pl.BlockSpec(memory_space=pltpu.SMEM)] + bands + [anywhere] * n_old,
        out_specs=anywhere,
        scratch_shapes=[pltpu.SemaphoreType.DMA((len(moves),))],
        input_output_aliases={1 + len(pieces): 0} if n_old else {},
    )(home, *pieces, *([] if earlier is None else [earlier]))


def on_device(prompt_rows, up_master, down_master, norm_gain):
    n_fs = lax.axis_size("fs")
    n_tp = lax.axis_size("tp")
    n_x = n_tp // 2
    half = n_fs // 2
    z = lax.axis_index("fs")
    tp = lax.axis_index("tp")
    x = tp // 2
    core = tp % 2
    direction = 1 - 2 * core
    home = jnp.stack([z, direction])

    up_rows, width = up_master.shape
    span = width // n_fs
    per_tp = n_fs // n_tp
    piece = per_tp * span
    down_cols = down_master.shape[1]
    full = down_cols * n_tp
    folds = down_cols // piece
    sides = full // width

    up_cast = (up_master * norm_gain[:, None]).astype(jnp.bfloat16)
    down_cast = down_master.astype(jnp.bfloat16)
    up_parts = up_cast.reshape(up_rows, per_tp, n_tp, span).transpose(2, 0, 1, 3)
    up_parts = up_parts.reshape(n_tp, 1, up_rows, piece)
    down_parts = down_cast.reshape(n_tp, span, folds, piece).transpose(0, 2, 1, 3)
    down_parts = down_parts.reshape(n_tp, 1, folds * span, piece)
    parts = jnp.concatenate([up_parts, down_parts], axis=1)
    pair = [(k, k ^ 1) for k in range(n_tp)]
    chips = [[2 * k + c for k in range(n_x)] for c in range(2)]
    parts = parts.reshape(n_x, 2, 2, *parts.shape[2:])
    parts = lax.all_to_all(
        parts, "tp", split_axis=0, concat_axis=0, tiled=True, axis_index_groups=chips
    )
    theirs = lax.ppermute(parts, "tp", pair)
    even = core == 0
    parts = jnp.stack([jnp.where(even, parts, theirs), jnp.where(even, theirs, parts)], axis=1)
    up_both = []
    down_both = []
    for group in (0, 1):
        chosen = jnp.where(even, parts[:, :, group], parts[:, :, 1 - group])
        chosen = chosen.reshape(n_tp, 2, *chosen.shape[3:])
        up_both.append(chosen[:, 0].transpose(1, 0, 2).reshape(up_rows, width))
        block = chosen[:, 1].reshape(sides, n_tp // sides, folds, span, piece)
        down_both.append(block.transpose(0, 3, 1, 2, 4).reshape(sides * span, width))

    ring = [
        (f * n_tp + k, (f + (1 if k % 2 == 0 else -1)) % n_fs * n_tp + k)
        for f in range(n_fs)
        for k in range(n_tp)
    ]
    up_msg = [jnp.concatenate(up_both, axis=0)]
    down_msg = [jnp.concatenate(down_both, axis=0)]
    last_sent = {}
    for step in range(1, half + 1):
        for name, msgs in (("up", up_msg), ("down", down_msg)):
            sent = msgs[-1]
            if step == half:
                sent = lax.optimization_barrier(sent[:up_rows])
                last_sent[name] = sent
            msgs.append(lax.ppermute(sent, ("fs", "tp"), ring))

    up = {-k: (up_msg[k], 0) for k in range(half)} | {half: (up_msg[half], 0)}
    down = {-k: (down_msg[k], 0) for k in range(half)} | {half: (down_msg[half], 0)}
    up[1 - half] = (last_sent["up"], 0)
    down[1 - half] = (last_sent["down"], 0)
    batches = [(1, half - 5), (half - 4, half - 3), (half - 2, half - 1)]
    for first, last in batches:
        steps = range(first, last + 1)
        bands = [m[k][up_rows:] for k in steps for m in (up_msg, down_msg)]
        got = lax.ppermute(jnp.concatenate(bands, axis=0), "tp", pair)
        for k in steps:
            up[k] = (got, 2 * (k - first) * up_rows)
            down[k] = (got, (2 * (k - first) + 1) * up_rows)

    def up_moves(keys):
        return [(up[k][0], up[k][1], up_rows, k, up_rows, 0, 0) for k in keys]

    def down_moves(keys):
        return [
            (down[k][0], down[k][1] + s * span, span, k, span, 0, s * width)
            for k in keys
            for s in range(sides)
        ]

    def within(least, most):
        return [k for k in sorted(up) if least <= abs(k) <= most]

    late = within(half - 2, half)
    up_shape = jax.ShapeDtypeStruct((n_fs * up_rows, width), jnp.bfloat16)
    down_shape = jax.ShapeDtypeStruct((n_fs * span, full), jnp.bfloat16)
    blank = jnp.zeros((up_rows, width), jnp.bfloat16)
    moves = up_moves(within(0, half - 3))
    moves += [(blank, 0, up_rows, k, up_rows, 0, 0) for k in late]
    up_sampler = place(home, moves, up_shape, n_fs)
    down_sampler = place(home, down_moves(within(0, half - 3)), down_shape, n_fs)

    tokens = prompt_rows.shape[0]
    block = tokens // n_tp
    order = [(dx % n_x, dc) for dc in (1, 0) for dx in range(1, n_x + 1)]
    rows = [
        lax.dynamic_slice_in_dim(
            prompt_rows, ((x + dx) % n_x * 2 + (core + dc) % 2) * block, block, axis=0
        )
        for dx, dc in order
    ]
    values = lax.optimization_barrier(jnp.concatenate(rows, axis=0)).astype(jnp.float32)
    scale = lax.rsqrt(jnp.mean(values * values, axis=-1, keepdims=True) + eps)
    normed = lax.optimization_barrier((values * scale).astype(jnp.bfloat16))
    pre_act = jnp.dot(normed, up_sampler, preferred_element_type=jnp.float32)
    pre_act = lax.optimization_barrier(pre_act)

    first = late[-1] - len(late) // 2
    rest = jnp.zeros((len(late) * up_rows, width), jnp.bfloat16)
    for k in sorted(late, key=lambda k: (abs(k), k > 0)):
        slot = (k * direction - first + 2 * n_fs) % n_fs
        band = up[k][0][up[k][1] : up[k][1] + up_rows]
        rest = lax.dynamic_update_slice_in_dim(rest, band, slot * up_rows, axis=0)
    ends = (len(late) - 1) * up_rows
    features = jnp.concatenate([normed, normed[:, :ends]], axis=1)
    features = lax.dynamic_slice_in_dim(
        features, (z + first) % n_fs * up_rows, len(late) * up_rows, axis=1
    )
    features = lax.optimization_barrier(features)
    pre_act = pre_act + jnp.dot(features, rest, preferred_element_type=jnp.float32)
    hidden = jnp.square(jax.nn.relu(pre_act)).astype(jnp.bfloat16)

    down_sampler = place(home, down_moves(late), down_shape, n_fs, down_sampler)
    up_sampler = place(home, up_moves(late), up_shape, n_fs, up_sampler)

    right = [(j, (j + 2) % n_tp) for j in range(n_tp)]
    left = [(j, (j - 2) % n_tp) for j in range(n_tp)]
    theirs = jnp.dot(hidden[: tokens // 2], down_sampler, preferred_element_type=jnp.float32)
    theirs = lax.ppermute(theirs.astype(jnp.bfloat16), "tp", pair)
    mine = jnp.dot(hidden[tokens // 2 :], down_sampler, preferred_element_type=jnp.float32)
    mine = lax.optimization_barrier(mine.astype(jnp.bfloat16))
    chip = mine.astype(jnp.float32) + theirs.astype(jnp.float32)
    after, across, before, total = [chip[k * block : (k + 1) * block] for k in range(n_x)]
    across = across.astype(jnp.bfloat16)
    mid = full // 2
    one = lax.ppermute(across[:, :mid], "tp", right).astype(jnp.float32)
    two = lax.ppermute(across[:, mid:], "tp", left).astype(jnp.float32)
    after = jnp.concatenate([after[:, :mid] + one, after[:, mid:]], axis=1)
    before = jnp.concatenate([before[:, :mid], before[:, mid:] + two], axis=1)
    after = lax.ppermute(after.astype(jnp.bfloat16), "tp", right).astype(jnp.float32)
    before = lax.ppermute(before.astype(jnp.bfloat16), "tp", left).astype(jnp.float32)
    total = (total + after + before).astype(jnp.bfloat16)
    return (up_sampler[None], down_sampler[None], total)


def solution(mesh):
    in_specs = (P(("grp", "fs"), None), P("fs", "tp"), P("fs", "tp"), P("fs"))
    out_specs = (
        P(("grp", "tp"), None, None),
        P(("grp", "tp"), None, None),
        P(("grp", "fs", "tp"), None),
    )

    return jax.shard_map(
        on_device, mesh=mesh, in_specs=in_specs, out_specs=out_specs, check_vma=False
    )
```

```python
import jax
import jax.numpy as jnp
from jax import lax
from jax.experimental import pallas as pl
from jax.experimental.pallas import tpu as pltpu
from jax.sharding import PartitionSpec as P


eps = 1e-06


def place(z, moves, outs, n_fs, earlier=None):
    pieces = []
    for move in moves:
        if not any(move[0] is piece for piece in pieces):
            pieces.append(move[0])
    at = [next(k for k, piece in enumerate(pieces) if piece is move[0]) for move in moves]
    n_old = 0 if earlier is None else len(earlier)

    def body(z_ref, *refs):
        ins = refs[: len(pieces)]
        out_refs = refs[len(pieces) + n_old : len(pieces) + n_old + len(outs)]
        sems = refs[-1]
        copies = []
        for k, (_, row, rows, out, offset, block, within, col) in enumerate(moves):
            home = lax.rem(z_ref[0] + (offset + n_fs), n_fs)
            start = pl.multiple_of(home * block + within, 16)
            src = ins[at[k]]
            dst = out_refs[out].at[pl.ds(start, rows), pl.ds(col, src.shape[1])]
            copies.append(pltpu.make_async_copy(src.at[pl.ds(row, rows)], dst, sems.at[k]))
        for copy in copies:
            copy.start()
        for copy in copies:
            copy.wait()

    anywhere = pl.BlockSpec(memory_space=pl.ANY)
    old = [] if earlier is None else list(earlier)
    return pl.pallas_call(
        body,
        out_shape=outs,
        in_specs=[pl.BlockSpec(memory_space=pltpu.SMEM)]
        + [pl.BlockSpec(memory_space=pltpu.VMEM)] * len(pieces)
        + [anywhere] * n_old,
        out_specs=[anywhere] * len(outs),
        scratch_shapes=[pltpu.SemaphoreType.DMA((len(moves),))],
        input_output_aliases={1 + len(pieces) + k: k for k in range(n_old)},
    )(z.reshape(1), *pieces, *old)


def on_device(prompt_rows, up_master, down_master, norm_gain):
    n_fs = lax.axis_size("fs")
    n_tp = lax.axis_size("tp")
    n_x = n_tp // 2
    half = n_fs // 2
    z = lax.axis_index("fs")
    tp = lax.axis_index("tp")
    x = tp // 2
    core = tp % 2

    up_rows, width = up_master.shape
    span = width // n_fs
    per_tp = n_fs // n_tp
    piece = per_tp * span
    down_cols = down_master.shape[1]
    full = down_cols * n_tp
    folds = down_cols // piece
    sides = full // width

    up_cast = (up_master * norm_gain[:, None]).astype(jnp.bfloat16)
    down_cast = down_master.astype(jnp.bfloat16)
    up_parts = up_cast.reshape(up_rows, per_tp, n_tp, span).transpose(2, 0, 1, 3)
    up_parts = up_parts.reshape(n_tp, 1, up_rows, piece)
    down_parts = down_cast.reshape(n_tp, span, folds, piece).transpose(0, 2, 1, 3)
    down_parts = down_parts.reshape(n_tp, 1, folds * span, piece)
    parts = jnp.concatenate([up_parts, down_parts], axis=1)
    parts = lax.all_to_all(parts, "tp", split_axis=0, concat_axis=0, tiled=True)
    up_own = parts[:, 0].transpose(1, 0, 2).reshape(up_rows, width)
    down_own = parts[:, 1].reshape(sides, n_tp // sides, folds, span, piece)
    down_own = down_own.transpose(0, 3, 1, 2, 4).reshape(sides * span, width)

    own = jnp.concatenate([up_own, down_own], axis=0)

    fore = [(k, (k + 1) % n_fs) for k in range(n_fs)]
    back = [(k, (k - 1) % n_fs) for k in range(n_fs)]
    held = {0: own}
    for step in range(1, half):
        held[-step] = lax.ppermute(held[1 - step], "fs", fore)
        held[step] = lax.ppermute(held[step - 1], "fs", back)
    up_far = lax.ppermute(held[1 - half][:up_rows], "fs", fore)
    down_far = lax.ppermute(held[half - 1][up_rows:], "fs", back)

    def up_moves(keys):
        return [(held[k], 0, up_rows, 0, k, up_rows, 0, 0) for k in keys]

    def down_moves(keys):
        return [
            (held[k], up_rows + s * span, span, 0, k, span, 0, s * width)
            for k in keys
            for s in range(sides)
        ]

    def within(least, most):
        return [k for k in held if least <= abs(k) <= most]

    late = [half - 2, half - 1, half, half + 1, half + 2]
    up_shape = [jax.ShapeDtypeStruct((n_fs * up_rows, width), jnp.bfloat16)]
    down_shape = [jax.ShapeDtypeStruct((n_fs * span, full), jnp.bfloat16)]
    blank = jnp.zeros((up_rows, width), jnp.bfloat16)
    moves = up_moves(within(0, half - 3))
    moves += [(blank, 0, up_rows, 0, k, up_rows, 0, 0) for k in late]
    up_sampler = place(z, moves, up_shape, n_fs)
    down_sampler = place(z, down_moves(within(0, half - 4)), down_shape, n_fs)
    moves = down_moves(within(half - 3, half - 2))
    down_sampler = place(z, moves, down_shape, n_fs, down_sampler)

    tokens = prompt_rows.shape[0]
    block = tokens // n_tp
    order = [(dx % n_x, dc) for dc in (1, 0) for dx in range(1, n_x + 1)]
    rows = [
        lax.dynamic_slice_in_dim(
            prompt_rows, ((x + dx) % n_x * 2 + (core + dc) % 2) * block, block, axis=0
        )
        for dx, dc in order
    ]
    values = lax.optimization_barrier(jnp.concatenate(rows, axis=0)).astype(jnp.float32)
    scale = lax.rsqrt(jnp.mean(values * values, axis=-1, keepdims=True) + eps)
    normed = lax.optimization_barrier((values * scale).astype(jnp.bfloat16))
    pre_act = jnp.dot(normed, up_sampler[0], preferred_element_type=jnp.float32)
    pre_act = lax.optimization_barrier(pre_act)

    rest = [up_far if k == half else held[k if k < half else k - n_fs][:up_rows] for k in late]
    rest = jnp.concatenate(rest, axis=0)
    ends = (len(late) - 1) * up_rows
    features = jnp.concatenate([normed, normed[:, :ends]], axis=1)
    features = lax.dynamic_slice_in_dim(
        features, (z + late[0]) % n_fs * up_rows, len(late) * up_rows, axis=1
    )
    features = lax.optimization_barrier(features)
    added = jnp.dot(features, rest, preferred_element_type=jnp.float32)
    pre_act = pre_act + lax.optimization_barrier(added)
    hidden = jnp.square(jax.nn.relu(pre_act)).astype(jnp.bfloat16)

    moves = down_moves(within(half - 1, half - 1))
    moves += [(down_far, k * span, span, 0, half, span, 0, k * width) for k in range(sides)]
    down_sampler = place(z, moves, down_shape, n_fs, down_sampler)[0]
    moves = up_moves(within(half - 2, half - 1))
    moves += [(up_far, 0, up_rows, 0, half, up_rows, 0, 0)]
    up_sampler = place(z, moves, up_shape, n_fs, up_sampler)[0]

    pair = [(k, k ^ 1) for k in range(n_tp)]
    right = [(j, (j + 2) % n_tp) for j in range(n_tp)]
    left = [(j, (j - 2) % n_tp) for j in range(n_tp)]
    bounds = [0, 3 * full // 8, full]
    summed = jnp.zeros((block, full), jnp.bfloat16)
    for lo, hi in zip(bounds[:-1], bounds[1:]):
        weights = lax.slice_in_dim(down_sampler, lo, hi, axis=1)
        partial = jnp.dot(hidden, weights, preferred_element_type=jnp.float32).astype(jnp.bfloat16)
        theirs = lax.ppermute(partial[: tokens // 2], "tp", pair)
        chip = partial[tokens // 2 :].astype(jnp.float32) + theirs.astype(jnp.float32)
        after, across, before, total = [chip[j * block : (j + 1) * block] for j in range(n_x)]
        across = across.astype(jnp.bfloat16)
        mid = (hi - lo) // 2
        ends = across[:, :mid], across[:, mid:]
        first = lax.ppermute(ends[0], "tp", right).astype(jnp.float32)
        second = lax.ppermute(ends[1], "tp", left).astype(jnp.float32)
        first = (after[:, :mid] + first).astype(jnp.bfloat16)
        second = (before[:, mid:] + second).astype(jnp.bfloat16)
        after = lax.dynamic_update_slice(after.astype(jnp.bfloat16), first, (0, 0))
        before = lax.dynamic_update_slice(before.astype(jnp.bfloat16), second, (0, mid))
        after = lax.ppermute(after, "tp", right).astype(jnp.float32)
        before = lax.ppermute(before, "tp", left).astype(jnp.float32)
        total = (total + after + before).astype(jnp.bfloat16)
        summed = lax.dynamic_update_slice(summed, total, (0, lo))
    return (up_sampler[None], down_sampler[None], summed)


def solution(mesh):
    in_specs = (P(("grp", "fs"), None), P("fs", "tp"), P("fs", "tp"), P("fs"))
    out_specs = (
        P(("grp", "tp"), None, None),
        P(("grp", "tp"), None, None),
        P(("grp", "fs", "tp"), None),
    )

    return jax.shard_map(
        on_device, mesh=mesh, in_specs=in_specs, out_specs=out_specs, check_vma=False
    )
```

```python
import jax
import jax.numpy as jnp
from jax import lax
from jax.experimental import pallas as pl
from jax.experimental.pallas import tpu as pltpu
from jax.sharding import PartitionSpec as P


eps = 1e-06


def place(z, moves, outs, n_fs, earlier=None):
    pieces = []
    for move in moves:
        if not any(move[0] is piece for piece in pieces):
            pieces.append(move[0])
    at = [next(k for k, piece in enumerate(pieces) if piece is move[0]) for move in moves]
    n_old = 0 if earlier is None else len(earlier)

    def body(z_ref, *refs):
        ins = refs[: len(pieces)]
        out_refs = refs[len(pieces) + n_old : len(pieces) + n_old + len(outs)]
        sems = refs[-1]
        copies = []
        for k, (_, row, rows, out, offset, block, within, col) in enumerate(moves):
            home = lax.rem(z_ref[0] + (offset + n_fs), n_fs)
            start = pl.multiple_of(home * block + within, 16)
            src = ins[at[k]]
            dst = out_refs[out].at[pl.ds(start, rows), pl.ds(col, src.shape[1])]
            copies.append(pltpu.make_async_copy(src.at[pl.ds(row, rows)], dst, sems.at[k]))
        for copy in copies:
            copy.start()
        for copy in copies:
            copy.wait()

    anywhere = pl.BlockSpec(memory_space=pl.ANY)
    old = [] if earlier is None else list(earlier)
    return pl.pallas_call(
        body,
        out_shape=outs,
        in_specs=[pl.BlockSpec(memory_space=pltpu.SMEM)]
        + [pl.BlockSpec(memory_space=pltpu.VMEM)] * len(pieces)
        + [anywhere] * n_old,
        out_specs=[anywhere] * len(outs),
        scratch_shapes=[pltpu.SemaphoreType.DMA((len(moves),))],
        input_output_aliases={1 + len(pieces) + k: k for k in range(n_old)},
    )(z.reshape(1), *pieces, *old)


def on_device(prompt_rows, up_master, down_master, norm_gain):
    n_fs = lax.axis_size("fs")
    n_tp = lax.axis_size("tp")
    n_x = n_tp // 2
    half = n_fs // 2
    z = lax.axis_index("fs")
    tp = lax.axis_index("tp")
    x = tp // 2
    core = tp % 2

    up_rows, width = up_master.shape
    span = width // n_fs
    per_tp = n_fs // n_tp
    piece = per_tp * span
    down_cols = down_master.shape[1]
    full = down_cols * n_tp
    folds = down_cols // piece
    sides = full // width

    up_cast = (up_master * norm_gain[:, None]).astype(jnp.bfloat16)
    down_cast = down_master.astype(jnp.bfloat16)
    up_parts = up_cast.reshape(up_rows, per_tp, n_tp, span).transpose(2, 0, 1, 3)
    up_parts = up_parts.reshape(n_tp, 1, up_rows, piece)
    down_parts = down_cast.reshape(n_tp, span, folds, piece).transpose(0, 2, 1, 3)
    down_parts = down_parts.reshape(n_tp, 1, folds * span, piece)
    parts = jnp.concatenate([up_parts, down_parts], axis=1)
    parts = lax.all_to_all(parts, "tp", split_axis=0, concat_axis=0, tiled=True)
    up_own = parts[:, 0].transpose(1, 0, 2).reshape(up_rows, width)
    down_own = parts[:, 1].reshape(sides, n_tp // sides, folds, span, piece)
    down_own = down_own.transpose(0, 3, 1, 2, 4).reshape(sides * span, width)

    own = jnp.concatenate([up_own, down_own], axis=0)

    fore = [(k, (k + 1) % n_fs) for k in range(n_fs)]
    back = [(k, (k - 1) % n_fs) for k in range(n_fs)]
    held = {0: own}
    for step in range(1, half):
        held[-step] = lax.ppermute(held[1 - step], "fs", fore)
        held[step] = lax.ppermute(held[step - 1], "fs", back)
    up_far = lax.ppermute(held[1 - half][:up_rows], "fs", fore)
    down_far = lax.ppermute(held[half - 1][up_rows:], "fs", back)

    def up_moves(keys):
        return [(held[k], 0, up_rows, 0, k, up_rows, 0, 0) for k in keys]

    def down_moves(keys):
        return [
            (held[k], up_rows + s * span, span, 0, k, span, 0, s * width)
            for k in keys
            for s in range(sides)
        ]

    def within(least, most):
        return [k for k in held if least <= abs(k) <= most]

    late = [half - 2, half - 1, half, half + 1, half + 2]
    up_shape = [jax.ShapeDtypeStruct((n_fs * up_rows, width), jnp.bfloat16)]
    down_shape = [jax.ShapeDtypeStruct((n_fs * span, full), jnp.bfloat16)]
    blank = jnp.zeros((up_rows, width), jnp.bfloat16)
    moves = up_moves(within(0, half - 3))
    moves += [(blank, 0, up_rows, 0, k, up_rows, 0, 0) for k in late]
    up_sampler = place(z, moves, up_shape, n_fs)
    down_sampler = place(z, down_moves(within(0, half - 4)), down_shape, n_fs)
    moves = down_moves(within(half - 3, half - 3))
    down_sampler = place(z, moves, down_shape, n_fs, down_sampler)

    tokens = prompt_rows.shape[0]
    block = tokens // n_tp
    order = [(dx % n_x, dc) for dc in (1, 0) for dx in range(1, n_x + 1)]
    rows = [
        lax.dynamic_slice_in_dim(
            prompt_rows, ((x + dx) % n_x * 2 + (core + dc) % 2) * block, block, axis=0
        )
        for dx, dc in order
    ]
    values = lax.optimization_barrier(jnp.concatenate(rows, axis=0)).astype(jnp.float32)
    scale = lax.rsqrt(jnp.mean(values * values, axis=-1, keepdims=True) + eps)
    normed = lax.optimization_barrier((values * scale).astype(jnp.bfloat16))
    pre_act = jnp.dot(normed, up_sampler[0], preferred_element_type=jnp.float32)
    pre_act = lax.optimization_barrier(pre_act)

    rest = jnp.zeros((len(late) * up_rows, width), jnp.bfloat16)
    for k in sorted(late, key=lambda k: k == half):
        band = up_far if k == half else held[k if k < half else k - n_fs][:up_rows]
        rest = lax.dynamic_update_slice(rest, band, ((k - late[0]) * up_rows, 0))
        if k != half:
            rest = lax.optimization_barrier(rest)
    ends = (len(late) - 1) * up_rows
    features = jnp.concatenate([normed, normed[:, :ends]], axis=1)
    features = lax.dynamic_slice_in_dim(
        features, (z + late[0]) % n_fs * up_rows, len(late) * up_rows, axis=1
    )
    features = lax.optimization_barrier(features)
    added = jnp.dot(features, rest, preferred_element_type=jnp.float32)
    pre_act = pre_act + lax.optimization_barrier(added)
    hidden = jnp.square(jax.nn.relu(pre_act)).astype(jnp.bfloat16)

    moves = down_moves(within(half - 2, half - 1))
    moves += [(down_far, k * span, span, 0, half, span, 0, k * width) for k in range(sides)]
    down_sampler = place(z, moves, down_shape, n_fs, down_sampler)[0]
    moves = up_moves(within(half - 2, half - 1))
    moves += [(up_far, 0, up_rows, 0, half, up_rows, 0, 0)]
    up_sampler = place(z, moves, up_shape, n_fs, up_sampler)[0]

    pair = [(k, k ^ 1) for k in range(n_tp)]
    right = [(j, (j + 2) % n_tp) for j in range(n_tp)]
    left = [(j, (j - 2) % n_tp) for j in range(n_tp)]
    bounds = [0, 3 * full // 8, full]
    summed = jnp.zeros((block, full), jnp.bfloat16)
    for lo, hi in zip(bounds[:-1], bounds[1:]):
        weights = lax.slice_in_dim(down_sampler, lo, hi, axis=1)
        partial = jnp.dot(hidden, weights, preferred_element_type=jnp.float32).astype(jnp.bfloat16)
        theirs = lax.ppermute(partial[: tokens // 2], "tp", pair)
        chip = partial[tokens // 2 :].astype(jnp.float32) + theirs.astype(jnp.float32)
        after, across, before, total = [chip[j * block : (j + 1) * block] for j in range(n_x)]
        across = across.astype(jnp.bfloat16)
        mid = (hi - lo) // 2
        ends = across[:, :mid], across[:, mid:]
        first = lax.ppermute(ends[0], "tp", right).astype(jnp.float32)
        second = lax.ppermute(ends[1], "tp", left).astype(jnp.float32)
        first = (after[:, :mid] + first).astype(jnp.bfloat16)
        second = (before[:, mid:] + second).astype(jnp.bfloat16)
        after = lax.dynamic_update_slice(after.astype(jnp.bfloat16), first, (0, 0))
        before = lax.dynamic_update_slice(before.astype(jnp.bfloat16), second, (0, mid))
        after = lax.ppermute(after, "tp", right).astype(jnp.float32)
        before = lax.ppermute(before, "tp", left).astype(jnp.float32)
        total = (total + after + before).astype(jnp.bfloat16)
        summed = lax.dynamic_update_slice(summed, total, (0, lo))
        if hi < full:
            summed = lax.optimization_barrier(summed)
    return (up_sampler[None], down_sampler[None], summed)


def solution(mesh):
    in_specs = (P(("grp", "fs"), None), P("fs", "tp"), P("fs", "tp"), P("fs"))
    out_specs = (
        P(("grp", "tp"), None, None),
        P(("grp", "tp"), None, None),
        P(("grp", "fs", "tp"), None),
    )

    return jax.shard_map(
        on_device, mesh=mesh, in_specs=in_specs, out_specs=out_specs, check_vma=False
    )
```

```python
import jax
import jax.numpy as jnp
from jax import lax
from jax.experimental import pallas as pl
from jax.experimental.pallas import tpu as pltpu
from jax.sharding import PartitionSpec as P


eps = 1e-06


def place(z, moves, outs, n_fs, earlier=None):
    pieces = []
    for move in moves:
        if not any(move[0] is piece for piece in pieces):
            pieces.append(move[0])
    at = [next(k for k, piece in enumerate(pieces) if piece is move[0]) for move in moves]
    n_old = 0 if earlier is None else len(earlier)

    def body(z_ref, *refs):
        ins = refs[: len(pieces)]
        out_refs = refs[len(pieces) + n_old : len(pieces) + n_old + len(outs)]
        sems = refs[-1]
        copies = []
        for k, (_, row, rows, out, offset, block, within, col) in enumerate(moves):
            home = lax.rem(z_ref[0] + (offset + n_fs), n_fs)
            start = pl.multiple_of(home * block + within, 16)
            src = ins[at[k]]
            dst = out_refs[out].at[pl.ds(start, rows), pl.ds(col, src.shape[1])]
            copies.append(pltpu.make_async_copy(src.at[pl.ds(row, rows)], dst, sems.at[k]))
        for copy in copies:
            copy.start()
        for copy in copies:
            copy.wait()

    anywhere = pl.BlockSpec(memory_space=pl.ANY)
    old = [] if earlier is None else list(earlier)
    return pl.pallas_call(
        body,
        out_shape=outs,
        in_specs=[pl.BlockSpec(memory_space=pltpu.SMEM)]
        + [pl.BlockSpec(memory_space=pltpu.VMEM)] * len(pieces)
        + [anywhere] * n_old,
        out_specs=[anywhere] * len(outs),
        scratch_shapes=[pltpu.SemaphoreType.DMA((len(moves),))],
        compiler_params=pltpu.CompilerParams(vmem_limit_bytes=12 * 2**20),
        input_output_aliases={1 + len(pieces) + k: k for k in range(n_old)},
    )(z.reshape(1), *pieces, *old)


def on_device(prompt_rows, up_master, down_master, norm_gain):
    n_fs = lax.axis_size("fs")
    n_tp = lax.axis_size("tp")
    n_x = n_tp // 2
    half = n_fs // 2
    z = lax.axis_index("fs")
    tp = lax.axis_index("tp")
    x = tp // 2
    core = tp % 2

    up_rows, width = up_master.shape
    span = width // n_fs
    per_tp = n_fs // n_tp
    piece = per_tp * span
    down_cols = down_master.shape[1]
    full = down_cols * n_tp
    folds = down_cols // piece
    sides = full // width

    up_cast = (up_master * norm_gain[:, None]).astype(jnp.bfloat16)
    down_cast = down_master.astype(jnp.bfloat16)
    up_parts = up_cast.reshape(up_rows, per_tp, n_tp, span).transpose(2, 0, 1, 3)
    up_parts = up_parts.reshape(n_tp, 1, up_rows, piece)
    down_parts = down_cast.reshape(n_tp, span, folds, piece).transpose(0, 2, 1, 3)
    down_parts = down_parts.reshape(n_tp, 1, folds * span, piece)
    parts = jnp.concatenate([up_parts, down_parts], axis=1)
    parts = lax.all_to_all(parts, "tp", split_axis=0, concat_axis=0, tiled=True)
    up_own = parts[:, 0].transpose(1, 0, 2).reshape(up_rows, width)
    down_own = parts[:, 1].reshape(sides, n_tp // sides, folds, span, piece)
    down_own = down_own.transpose(0, 3, 1, 2, 4).reshape(sides * span, width)

    own = jnp.concatenate([up_own, down_own], axis=0)

    fore = [(k, (k + 1) % n_fs) for k in range(n_fs)]
    back = [(k, (k - 1) % n_fs) for k in range(n_fs)]
    held = {0: own}
    for step in range(1, half):
        held[-step] = lax.ppermute(held[1 - step], "fs", fore)
        held[step] = lax.ppermute(held[step - 1], "fs", back)
    up_far = lax.ppermute(held[1 - half][:up_rows], "fs", fore)
    down_far = lax.ppermute(held[half - 1][up_rows:], "fs", back)

    def up_moves(keys):
        return [(held[k], 0, up_rows, 0, k, up_rows, 0, 0) for k in keys]

    def down_moves(keys):
        return [
            (held[k], up_rows + s * span, span, 0, k, span, 0, s * width)
            for k in keys
            for s in range(sides)
        ]

    def within(least, most):
        return [k for k in held if least <= abs(k) <= most]

    late = [half - 2, half - 1, half, half + 1, half + 2]
    up_shape = [jax.ShapeDtypeStruct((n_fs * up_rows, width), jnp.bfloat16)]
    down_shape = [jax.ShapeDtypeStruct((n_fs * span, full), jnp.bfloat16)]
    blank = jnp.zeros((up_rows, width), jnp.bfloat16)
    moves = up_moves(within(0, half - 3))
    moves += [(blank, 0, up_rows, 0, k, up_rows, 0, 0) for k in late]
    up_sampler = place(z, moves, up_shape, n_fs)
    down_sampler = place(z, down_moves(within(0, half - 4)), down_shape, n_fs)
    moves = down_moves(within(half - 3, half - 3))
    down_sampler = place(z, moves, down_shape, n_fs, down_sampler)

    tokens = prompt_rows.shape[0]
    block = tokens // n_tp
    order = [(dx % n_x, dc) for dc in (1, 0) for dx in range(1, n_x + 1)]
    rows = [
        lax.dynamic_slice_in_dim(
            prompt_rows, ((x + dx) % n_x * 2 + (core + dc) % 2) * block, block, axis=0
        )
        for dx, dc in order
    ]
    values = lax.optimization_barrier(jnp.concatenate(rows, axis=0)).astype(jnp.float32)
    scale = lax.rsqrt(jnp.mean(values * values, axis=-1, keepdims=True) + eps)
    normed = lax.optimization_barrier((values * scale).astype(jnp.bfloat16))
    pre_act = jnp.dot(normed, up_sampler[0], preferred_element_type=jnp.float32)
    pre_act = lax.optimization_barrier(pre_act)

    rest = jnp.zeros((len(late) * up_rows, width), jnp.bfloat16)
    for k in sorted(late, key=lambda k: k == half):
        band = up_far if k == half else held[k if k < half else k - n_fs][:up_rows]
        rest = lax.dynamic_update_slice(rest, band, ((k - late[0]) * up_rows, 0))
        if k != half:
            rest = lax.optimization_barrier(rest)
    ends = (len(late) - 1) * up_rows
    features = jnp.concatenate([normed, normed[:, :ends]], axis=1)
    features = lax.dynamic_slice_in_dim(
        features, (z + late[0]) % n_fs * up_rows, len(late) * up_rows, axis=1
    )
    features = lax.optimization_barrier(features)
    pre_act = pre_act + jnp.dot(features, rest, preferred_element_type=jnp.float32)
    hidden = jnp.square(jax.nn.relu(pre_act)).astype(jnp.bfloat16)

    moves = down_moves(within(half - 2, half - 1))
    down_sampler = place(z, moves, down_shape, n_fs, down_sampler)
    moves = [(down_far, k * span, span, 0, half, span, 0, k * width) for k in range(sides)]
    down_sampler = place(z, moves, down_shape, n_fs, down_sampler)[0]
    moves = up_moves(within(half - 2, half - 1))
    moves += [(up_far, 0, up_rows, 0, half, up_rows, 0, 0)]
    up_sampler = place(z, moves, up_shape, n_fs, up_sampler)[0]

    pair = [(k, k ^ 1) for k in range(n_tp)]
    right = [(j, (j + 2) % n_tp) for j in range(n_tp)]
    left = [(j, (j - 2) % n_tp) for j in range(n_tp)]
    bounds = [0, 5 * full // 8, full]
    summed = jnp.zeros((block, full), jnp.bfloat16)
    for lo, hi in zip(bounds[:-1], bounds[1:]):
        weights = lax.slice_in_dim(down_sampler, lo, hi, axis=1)
        partial = jnp.dot(hidden, weights, preferred_element_type=jnp.float32).astype(jnp.bfloat16)
        theirs = lax.ppermute(partial[: tokens // 2], "tp", pair)
        chip = partial[tokens // 2 :].astype(jnp.float32) + theirs.astype(jnp.float32)
        after, across, before, total = [chip[j * block : (j + 1) * block] for j in range(n_x)]
        across = across.astype(jnp.bfloat16)
        mid = (hi - lo) // 2
        ends = across[:, :mid], across[:, mid:]
        first = lax.ppermute(ends[0], "tp", right).astype(jnp.float32)
        second = lax.ppermute(ends[1], "tp", left).astype(jnp.float32)
        first = (after[:, :mid] + first).astype(jnp.bfloat16)
        second = (before[:, mid:] + second).astype(jnp.bfloat16)
        after = lax.dynamic_update_slice(after.astype(jnp.bfloat16), first, (0, 0))
        before = lax.dynamic_update_slice(before.astype(jnp.bfloat16), second, (0, mid))
        after = lax.ppermute(after, "tp", right).astype(jnp.float32)
        before = lax.ppermute(before, "tp", left).astype(jnp.float32)
        total = (total + after + before).astype(jnp.bfloat16)
        summed = lax.dynamic_update_slice(summed, total, (0, lo))
        if hi < full:
            summed = lax.optimization_barrier(summed)
    return (up_sampler[None], down_sampler[None], summed)


def solution(mesh):
    in_specs = (P(("grp", "fs"), None), P("fs", "tp"), P("fs", "tp"), P("fs"))
    out_specs = (
        P(("grp", "tp"), None, None),
        P(("grp", "tp"), None, None),
        P(("grp", "fs", "tp"), None),
    )

    return jax.shard_map(
        on_device, mesh=mesh, in_specs=in_specs, out_specs=out_specs, check_vma=False
    )
```

```python
import jax
import jax.numpy as jnp
from jax import lax
from jax.experimental import pallas as pl
from jax.experimental.pallas import tpu as pltpu
from jax.sharding import PartitionSpec as P


eps = 1e-06


def place(z, moves, outs, n_fs, earlier=None):
    pieces = []
    for move in moves:
        if not any(move[0] is piece for piece in pieces):
            pieces.append(move[0])
    at = [next(k for k, piece in enumerate(pieces) if piece is move[0]) for move in moves]
    n_old = 0 if earlier is None else len(earlier)

    def body(z_ref, *refs):
        ins = refs[: len(pieces)]
        out_refs = refs[len(pieces) + n_old : len(pieces) + n_old + len(outs)]
        sems = refs[-1]
        copies = []
        for k, (_, row, rows, out, offset, block, within, col) in enumerate(moves):
            home = lax.rem(z_ref[0] + (offset + n_fs), n_fs)
            start = pl.multiple_of(home * block + within, 16)
            src = ins[at[k]]
            dst = out_refs[out].at[pl.ds(start, rows), pl.ds(col, src.shape[1])]
            copies.append(pltpu.make_async_copy(src.at[pl.ds(row, rows)], dst, sems.at[k]))
        for copy in copies:
            copy.start()
        for copy in copies:
            copy.wait()

    anywhere = pl.BlockSpec(memory_space=pl.ANY)
    old = [] if earlier is None else list(earlier)
    return pl.pallas_call(
        body,
        out_shape=outs,
        in_specs=[pl.BlockSpec(memory_space=pltpu.SMEM)]
        + [pl.BlockSpec(memory_space=pltpu.VMEM)] * len(pieces)
        + [anywhere] * n_old,
        out_specs=[anywhere] * len(outs),
        scratch_shapes=[pltpu.SemaphoreType.DMA((len(moves),))],
        compiler_params=pltpu.CompilerParams(vmem_limit_bytes=12 * 2**20),
        input_output_aliases={1 + len(pieces) + k: k for k in range(n_old)},
    )(z.reshape(1), *pieces, *old)


def on_device(prompt_rows, up_master, down_master, norm_gain):
    n_fs = lax.axis_size("fs")
    n_tp = lax.axis_size("tp")
    n_x = n_tp // 2
    half = n_fs // 2
    z = lax.axis_index("fs")
    tp = lax.axis_index("tp")
    x = tp // 2
    core = tp % 2

    up_rows, width = up_master.shape
    span = width // n_fs
    per_tp = n_fs // n_tp
    piece = per_tp * span
    down_cols = down_master.shape[1]
    full = down_cols * n_tp
    folds = down_cols // piece
    sides = full // width

    up_cast = (up_master * norm_gain[:, None]).astype(jnp.bfloat16)
    down_cast = down_master.astype(jnp.bfloat16)
    up_parts = up_cast.reshape(up_rows, per_tp, n_tp, span).transpose(2, 0, 1, 3)
    up_parts = up_parts.reshape(n_tp, 1, up_rows, piece)
    down_parts = down_cast.reshape(n_tp, span, folds, piece).transpose(0, 2, 1, 3)
    down_parts = down_parts.reshape(n_tp, 1, folds * span, piece)
    parts = jnp.concatenate([up_parts, down_parts], axis=1)
    parts = lax.all_to_all(parts, "tp", split_axis=0, concat_axis=0, tiled=True)
    up_own = parts[:, 0].transpose(1, 0, 2).reshape(up_rows, width)
    down_own = parts[:, 1].reshape(sides, n_tp // sides, folds, span, piece)
    down_own = down_own.transpose(0, 3, 1, 2, 4).reshape(sides * span, width)

    own = jnp.concatenate([up_own, down_own], axis=0)

    fore = [(k, (k + 1) % n_fs) for k in range(n_fs)]
    back = [(k, (k - 1) % n_fs) for k in range(n_fs)]
    held = {0: own}
    for step in range(1, half):
        held[-step] = lax.ppermute(held[1 - step], "fs", fore)
        held[step] = lax.ppermute(held[step - 1], "fs", back)
    up_far = lax.ppermute(held[1 - half][:up_rows], "fs", fore)
    down_far = lax.ppermute(held[half - 1][up_rows:], "fs", back)

    def up_moves(keys):
        return [(held[k], 0, up_rows, 0, k, up_rows, 0, 0) for k in keys]

    def down_moves(keys):
        return [
            (held[k], up_rows + s * span, span, 0, k, span, 0, s * width)
            for k in keys
            for s in range(sides)
        ]

    def within(least, most):
        return [k for k in held if least <= abs(k) <= most]

    late = [half - 2, half - 1, half, half + 1, half + 2]
    up_shape = [jax.ShapeDtypeStruct((n_fs * up_rows, width), jnp.bfloat16)]
    down_shape = [jax.ShapeDtypeStruct((n_fs * span, full), jnp.bfloat16)]
    blank = jnp.zeros((up_rows, width), jnp.bfloat16)
    moves = up_moves(within(0, half - 3))
    moves += [(blank, 0, up_rows, 0, k, up_rows, 0, 0) for k in late]
    up_sampler = place(z, moves, up_shape, n_fs)
    down_sampler = place(z, down_moves(within(0, half - 4)), down_shape, n_fs)
    moves = down_moves(within(half - 3, half - 3))
    down_sampler = place(z, moves, down_shape, n_fs, down_sampler)

    tokens = prompt_rows.shape[0]
    block = tokens // n_tp
    order = [(dx % n_x, dc) for dc in (1, 0) for dx in range(1, n_x + 1)]
    rows = [
        lax.dynamic_slice_in_dim(
            prompt_rows, ((x + dx) % n_x * 2 + (core + dc) % 2) * block, block, axis=0
        )
        for dx, dc in order
    ]
    values = lax.optimization_barrier(jnp.concatenate(rows, axis=0)).astype(jnp.float32)
    scale = lax.rsqrt(jnp.mean(values * values, axis=-1, keepdims=True) + eps)
    normed = lax.optimization_barrier((values * scale).astype(jnp.bfloat16))
    pre_act = jnp.dot(normed, up_sampler[0], preferred_element_type=jnp.float32)
    pre_act = lax.optimization_barrier(pre_act)

    rest = jnp.zeros((len(late) * up_rows, width), jnp.bfloat16)
    for k in sorted(late, key=lambda k: k == half):
        band = up_far if k == half else held[k if k < half else k - n_fs][:up_rows]
        rest = lax.dynamic_update_slice(rest, band, ((k - late[0]) * up_rows, 0))
        if k != half:
            rest = lax.optimization_barrier(rest)
    ends = (len(late) - 1) * up_rows
    features = jnp.concatenate([normed, normed[:, :ends]], axis=1)
    features = lax.dynamic_slice_in_dim(
        features, (z + late[0]) % n_fs * up_rows, len(late) * up_rows, axis=1
    )
    features = lax.optimization_barrier(features)
    pre_act = pre_act + jnp.dot(features, rest, preferred_element_type=jnp.float32)
    hidden = jnp.square(jax.nn.relu(pre_act)).astype(jnp.bfloat16)

    moves = down_moves(within(half - 2, half - 1))
    down_sampler = place(z, moves, down_shape, n_fs, down_sampler)
    moves = [(down_far, k * span, span, 0, half, span, 0, k * width) for k in range(sides)]
    down_sampler = place(z, moves, down_shape, n_fs, down_sampler)[0]
    moves = up_moves(within(half - 2, half - 1))
    moves += [(up_far, 0, up_rows, 0, half, up_rows, 0, 0)]
    up_sampler = place(z, moves, up_shape, n_fs, up_sampler)[0]

    pair = [(k, k ^ 1) for k in range(n_tp)]
    right = [(j, (j + 2) % n_tp) for j in range(n_tp)]
    left = [(j, (j - 2) % n_tp) for j in range(n_tp)]
    bounds = [0, 3 * full // 8, full]
    summed = jnp.zeros((block, full), jnp.bfloat16)
    for lo, hi in zip(bounds[:-1], bounds[1:]):
        weights = lax.slice_in_dim(down_sampler, lo, hi, axis=1)
        theirs = jnp.dot(hidden[: tokens // 2], weights, preferred_element_type=jnp.float32)
        theirs = theirs.astype(jnp.bfloat16)
        theirs = lax.ppermute(theirs, "tp", pair)
        mine = jnp.dot(hidden[tokens // 2 :], weights, preferred_element_type=jnp.float32)
        mine = lax.optimization_barrier(mine.astype(jnp.bfloat16))
        chip = mine.astype(jnp.float32) + theirs.astype(jnp.float32)
        after, across, before, total = [chip[j * block : (j + 1) * block] for j in range(n_x)]
        across = across.astype(jnp.bfloat16)
        mid = (hi - lo) // 2
        ends = across[:, :mid], across[:, mid:]
        first = lax.ppermute(ends[0], "tp", right).astype(jnp.float32)
        second = lax.ppermute(ends[1], "tp", left).astype(jnp.float32)
        first = (after[:, :mid] + first).astype(jnp.bfloat16)
        second = (before[:, mid:] + second).astype(jnp.bfloat16)
        after = lax.dynamic_update_slice(after.astype(jnp.bfloat16), first, (0, 0))
        before = lax.dynamic_update_slice(before.astype(jnp.bfloat16), second, (0, mid))
        after = lax.ppermute(after, "tp", right).astype(jnp.float32)
        before = lax.ppermute(before, "tp", left).astype(jnp.float32)
        total = (total + after + before).astype(jnp.bfloat16)
        summed = lax.dynamic_update_slice(summed, total, (0, lo))
        if hi < full:
            summed = lax.optimization_barrier(summed)
    return (up_sampler[None], down_sampler[None], summed)


def solution(mesh):
    in_specs = (P(("grp", "fs"), None), P("fs", "tp"), P("fs", "tp"), P("fs"))
    out_specs = (
        P(("grp", "tp"), None, None),
        P(("grp", "tp"), None, None),
        P(("grp", "fs", "tp"), None),
    )

    return jax.shard_map(
        on_device, mesh=mesh, in_specs=in_specs, out_specs=out_specs, check_vma=False
    )
```
